32 devices in a mesh: sp: 8 (over z, y), tp: 4 (over x, core).
Axes of the slice: x: 2, y: 2, z: 4, core: 2. Of those that a mesh axis runs over, the one named last changes fastest.
Arguments:
- residual_in: bfloat16 [6144, 2048], P('sp', 'tp'), may hold values from -11 to 11
- queries: bfloat16 [6144, 1024], P('sp', 'tp'), may hold values from -6 to 6
- keys: bfloat16 [6144, 256], P('sp'), may hold values from -6 to 6
- values: bfloat16 [6144, 256], P('sp'), may hold values from -6 to 6
- query_gain: float32 [128], replicated, may hold values from 1.5 to 5
- key_norm_gain: float32 [128], replicated, may hold values from 1.5 to 5
- out_weight: bfloat16 [1024, 2048], P('tp'), may hold values from -0.1875 to 0.1875
- mlp_gain: float32 [2048], replicated, may hold values from 0.1 to 1.9
- gate_weight: bfloat16 [2048, 5632], P('sp', 'tp'), may hold values from -0.125 to 0.125
- up_weight: bfloat16 [2048, 5632], P('sp', 'tp'), may hold values from -0.125 to 0.125
- down_weight: bfloat16 [5632, 2048], P('tp', 'sp'), may hold values from -0.15625 to 0.15625
Outputs:
- layer_out: bfloat16 [6144, 2048], P('sp', 'tp')
The draws below stay inside these ranges and needn't reach their ends.
All inputs are finite; a program needn't handle non-finite values.
Results may differ from the reference program's by a relative error of at most 0.012.
The reference program's roundings to bfloat16 on the way count: a program that leaves them out, or rounds other values in their place, can miss the bound.
Values may be sent and summed in bfloat16 or wider, within the bound.
A program may use at most 64 MiB of HBM per device.

```python
import math
import jax
import jax.numpy as jnp
from jax import lax

D = 2048
HEAD_SIZE = 128
QUERY_HEADS = 8
KEY_VALUE_HEADS = 2
FF = 5632
GRID = 64
TOK_DEV = 768
SEQUENCE_TOKENS = 6144
N_TP = 4


def draw_residual_in(key, part):
    column_scale = 0.5 * 4.0 ** (jnp.arange(D, dtype=jnp.float32) / D)
    rotary_period = jnp.clip(jax.random.normal(jax.random.fold_in(key, 3), (SEQUENCE_TOKENS, D)), -4.0, 4.0)
    return (rotary_period * column_scale).astype(jnp.bfloat16)


def draw_queries(key, part):
    rotary_period = jnp.clip(jax.random.normal(jax.random.fold_in(key, 1), (SEQUENCE_TOKENS, QUERY_HEADS * HEAD_SIZE)), -4.0, 4.0)
    return jnp.clip(rotary_period, -6.0, 6.0).astype(jnp.bfloat16)


def draw_keys(key, part):
    rotary_period = jnp.clip(jax.random.normal(jax.random.fold_in(key, 2), (SEQUENCE_TOKENS, KEY_VALUE_HEADS * HEAD_SIZE)), -4.0, 4.0)
    return jnp.clip(rotary_period, -6.0, 6.0).astype(jnp.bfloat16)


def draw_gain(key, salt):
    return jnp.exp(jax.random.uniform(jax.random.fold_in(key, salt), (HEAD_SIZE,), jnp.float32, math.log(1.5), math.log(3.0)))


def draw_query_gain(key, part):
    return draw_gain(key, 4)


def draw_key_norm_gain(key, part):
    return draw_gain(key, 5)


def steps_of(stream_key, extent, cuts, low, top_value):
    loudness, own = 1.0, jax.random.fold_in(stream_key, 6)
    for dim, shards_of in cuts:
        steps = jnp.exp(jax.random.uniform(jax.random.fold_in(own, dim), (shards_of,), jnp.float32, low / len(cuts), top_value / len(cuts)))
        loudness = loudness * jnp.repeat(steps, extent[dim] // shards_of).reshape([-1 if axis == dim else 1 for axis in range(len(extent))])
    return loudness


def gaussian(key, extent, spread, limit, cuts=(), kind=jnp.bfloat16):
    drawn = jax.random.normal(key, extent, jnp.float32) * spread
    if len(cuts) > 0:
        drawn = steps_of(key, extent, cuts, -0.22, 0.18) * drawn
    return jnp.clip(drawn, min=-limit, max=limit).astype(kind)


def setup_inputs(seed: int = 0) -> dict:
    key_of = jax.random.split(jax.random.key(seed), 12)
    return {
        "residual_in": draw_residual_in(jax.random.fold_in(key_of[11], 71), 0),
        "queries": draw_queries(jax.random.fold_in(key_of[11], 71), 0),
        "keys": draw_keys(jax.random.fold_in(key_of[11], 71), 0),
        "values": gaussian(key_of[3], (SEQUENCE_TOKENS, KEY_VALUE_HEADS * HEAD_SIZE), 1.0, 6.0, ((0, 8),)),
        "query_gain": draw_query_gain(jax.random.fold_in(key_of[11], 71), 0),
        "key_norm_gain": draw_key_norm_gain(jax.random.fold_in(key_of[11], 71), 0),
        "out_weight": gaussian(key_of[6], (QUERY_HEADS * HEAD_SIZE, D), (QUERY_HEADS * HEAD_SIZE) ** -0.5, 0.1875, ((0, 4),)),
        "mlp_gain": jnp.clip(1.0 + 0.18 * jax.random.normal(key_of[7], (D,), jnp.float32), 0.1, 1.9),
        "gate_weight": gaussian(key_of[8], (D, FF), D ** -0.5, 0.125, ((0, 8), (1, 4))),
        "up_weight": gaussian(key_of[9], (D, FF), D ** -0.5, 0.125, ((0, 8), (1, 4))),
        "down_weight": gaussian(key_of[10], (FF, D), (FF // 4) ** -0.5, 0.15625, ((0, 4), (1, 8))),
    }


eps = 1e-06
rotary_base = 10000.0

def apply_rotary(vectors, grid_positions):
    half_size = vectors.shape[-1] // 2
    frequency = rotary_base ** (-jnp.arange(0, half_size, 2, dtype=jnp.float32) / half_size)
    grid_row = (grid_positions // GRID).astype(jnp.float32)
    grid_col = (grid_positions % GRID).astype(jnp.float32)
    angles = jnp.concatenate([grid_row[:, None] * frequency, grid_col[:, None] * frequency], axis=-1)[:, None, :]
    cosine_table = jnp.cos(angles)
    sine_table = jnp.sin(angles)
    first_half = vectors[..., :half_size]
    second_half = vectors[..., half_size:]
    return jnp.concatenate([first_half * cosine_table - second_half * sine_table, first_half * sine_table + second_half * cosine_table], axis=-1)

def per_head_norm(vectors, gain):
    return vectors * lax.rsqrt(lax.optimization_barrier(jnp.mean(vectors * vectors, axis=-1, keepdims=True)) + eps) * gain

def grouped_sum(left, right, groups):
    group_width = left.shape[1] // groups

    def add_group(running, group_index):
        left_part = lax.dynamic_slice_in_dim(left, group_index * group_width, group_width, 1)
        right_part = lax.dynamic_slice_in_dim(right, group_index * group_width, group_width, 0)
        partial_sum = jnp.dot(left_part, right_part, preferred_element_type=jnp.float32)
        rounded = lax.optimization_barrier(partial_sum.astype(jnp.bfloat16))
        return (running + rounded.astype(jnp.float32), None)
    start_value = jnp.zeros((left.shape[0], right.shape[1]), jnp.float32)
    result, ignored = lax.scan(add_group, start_value, jnp.arange(groups, dtype=jnp.int32))
    return result

def reference(residual_in, queries, keys, values, query_gain, key_norm_gain, out_weight, mlp_gain, gate_weight, up_weight, down_weight):
    grid_positions = jnp.arange(SEQUENCE_TOKENS, dtype=jnp.int32)
    queries_per_group = QUERY_HEADS // KEY_VALUE_HEADS
    query_rows = apply_rotary(per_head_norm(queries.astype(jnp.float32).reshape(SEQUENCE_TOKENS, QUERY_HEADS, HEAD_SIZE), query_gain), grid_positions).astype(jnp.bfloat16)
    key_matrix = apply_rotary(per_head_norm(keys.astype(jnp.float32).reshape(SEQUENCE_TOKENS, KEY_VALUE_HEADS, HEAD_SIZE), key_norm_gain), grid_positions).astype(jnp.bfloat16)
    value_matrix = values.reshape(SEQUENCE_TOKENS, KEY_VALUE_HEADS, HEAD_SIZE)
    score_scale = HEAD_SIZE ** (-0.5)

    def one_head(head_index):
        head_queries = lax.dynamic_index_in_dim(query_rows, head_index, 1, keepdims=False)
        shared = head_index // queries_per_group
        head_keys = lax.dynamic_index_in_dim(key_matrix, shared, 1, keepdims=False)
        head_values = lax.dynamic_index_in_dim(value_matrix, shared, 1, keepdims=False)

        def one_block(first_row):
            block_queries = lax.dynamic_slice_in_dim(head_queries, first_row, TOK_DEV, 0)
            scores = jnp.dot(block_queries, head_keys.T, preferred_element_type=jnp.float32) * score_scale
            row_max = lax.optimization_barrier(jnp.max(scores, axis=1, keepdims=True))
            weights = jnp.exp(scores - row_max)
            row_sum = lax.optimization_barrier(jnp.sum(weights, axis=1, keepdims=True))
            weighted = jnp.dot(weights.astype(jnp.bfloat16), head_values, preferred_element_type=jnp.float32)
            return (weighted / row_sum).astype(jnp.bfloat16)
        starts = jnp.arange(0, SEQUENCE_TOKENS, TOK_DEV, dtype=jnp.int32)
        return lax.map(one_block, starts).reshape(SEQUENCE_TOKENS, HEAD_SIZE)
    heads_out = lax.map(one_head, jnp.arange(QUERY_HEADS, dtype=jnp.int32))
    attended = jnp.transpose(heads_out, (1, 0, 2)).reshape(SEQUENCE_TOKENS, QUERY_HEADS * HEAD_SIZE)
    projected = grouped_sum(attended, out_weight, N_TP)
    residual_mid = residual_in.astype(jnp.float32) + projected
    normed = (residual_mid * lax.rsqrt(lax.optimization_barrier(jnp.mean(residual_mid * residual_mid, axis=1, keepdims=True)) + eps) * mlp_gain).astype(jnp.bfloat16)
    gate_out = jnp.dot(normed, gate_weight, preferred_element_type=jnp.float32)
    up_out = jnp.dot(normed, up_weight, preferred_element_type=jnp.float32)
    hidden = (jax.nn.silu(gate_out) * up_out).astype(jnp.bfloat16)
    down_sum = grouped_sum(hidden, down_weight, N_TP)
    return (residual_mid + 0.5 * down_sum).astype(jnp.bfloat16)
```

```python
import functools
import jax
import jax.numpy as jnp
from jax import lax
from jax.experimental import pallas as pl
from jax.experimental.pallas import tpu as pltpu
from jax.sharding import PartitionSpec as P

D = 2048
HEAD_SIZE = 128
QUERY_HEADS = 8
KEY_VALUE_HEADS = 2
GRID = 64

eps = 1e-06
rotary_base = 10000.0
MESH = pl.DeviceIdType.MESH
VMEM_LIMIT = 60 * 1024 * 1024
F32 = jnp.float32
BF16 = jnp.bfloat16


def apply_rotary(vectors, grid_positions):
    half_size = vectors.shape[-1] // 2
    frequency = rotary_base ** (-jnp.arange(0, half_size, 2, dtype=F32) / half_size)
    grid_row = (grid_positions // GRID).astype(F32)
    grid_col = (grid_positions % GRID).astype(F32)
    angles = jnp.concatenate(
        [grid_row[:, None] * frequency, grid_col[:, None] * frequency], axis=-1
    )[:, None, :]
    cosine_table = jnp.cos(angles)
    sine_table = jnp.sin(angles)
    first_half = vectors[..., :half_size]
    second_half = vectors[..., half_size:]
    return jnp.concatenate(
        [
            first_half * cosine_table - second_half * sine_table,
            first_half * sine_table + second_half * cosine_table,
        ],
        axis=-1,
    )


def per_head_norm(vectors, gain):
    return vectors * lax.rsqrt(jnp.mean(vectors * vectors, axis=-1, keepdims=True) + eps) * gain


def remote(src, dst, send, recv, sp, tp):
    copy = pltpu.make_async_remote_copy(
        src_ref=src, dst_ref=dst, send_sem=send, recv_sem=recv,
        device_id={"sp": sp, "tp": tp}, device_id_type=MESH,
    )
    copy.start()
    return copy


def greet(peers):
    barrier = pltpu.get_barrier_semaphore()
    for sp, tp in peers:
        pl.semaphore_signal(
            barrier, inc=1, device_id={"sp": sp, "tp": tp}, device_id_type=MESH
        )
    pl.semaphore_wait(barrier, len(peers))


def place():
    sp = lax.axis_index("sp")
    tp = lax.axis_index("tp")
    return sp, tp, sp // 2, lax.rem(sp, 2), tp // 2, lax.rem(tp, 2)


def gather_kernel(nz, kv_ref, out_ref, sz, rz, sy, ry, sc, rc):
    sp, tp, z, y, x, c = place()
    rows = kv_ref.shape[0]
    half = rows // 2
    other = x * 2 + (1 - c)
    z_peers = [lax.rem(z + k, nz) * 2 + y for k in range(1, nz)]
    y_peer = z * 2 + 1 - y
    greet([(p, tp) for p in z_peers] + [(y_peer, tp), (sp, other)])

    def spot(owner):
        return out_ref.at[pl.ds(pl.multiple_of(owner * rows + c * half, half), half), :]

    own = kv_ref.at[pl.ds(pl.multiple_of(c * half, half), half), :]
    sends = []
    to_z = [
        remote(own, spot(sp), sz.at[k - 1], rz.at[k - 1], z_peers[k - 1], tp)
        for k in range(1, nz)
    ]
    to_y = [remote(own, spot(sp), sy.at[0], ry.at[0], y_peer, tp)]
    out_ref[pl.ds(pl.multiple_of(sp * rows, rows), rows), :] = kv_ref[...]
    to_core = []
    for k in range(1, nz):
        to_z[k - 1].wait_recv()
        block = spot(lax.rem(z - k + nz, nz) * 2 + y)
        to_y.append(remote(block, block, sy.at[k], ry.at[k], y_peer, tp))
        to_core.append(remote(block, block, sc.at[k - 1], rc.at[k - 1], sp, other))
    for k in range(nz):
        to_y[k].wait_recv()
        block = spot(lax.rem(z - k + nz, nz) * 2 + 1 - y)
        slot = nz - 1 + k
        to_core.append(remote(block, block, sc.at[slot], rc.at[slot], sp, other))
    for copy in to_core:
        copy.wait_recv()
    for copy in to_z + to_y + to_core:
        copy.wait_send()


def gather_keys(kv, n_sp):
    nz = n_sp // 2
    dma = pltpu.SemaphoreType.DMA
    return pl.pallas_call(
        functools.partial(gather_kernel, nz),
        out_shape=jax.ShapeDtypeStruct((n_sp * kv.shape[0], kv.shape[1]), kv.dtype),
        in_specs=[pl.BlockSpec(memory_space=pltpu.VMEM)],
        out_specs=pl.BlockSpec(memory_space=pltpu.VMEM),
        scratch_shapes=[dma((nz - 1,)), dma((nz - 1,)), dma((nz,)), dma((nz,)),
                        dma((2 * nz - 1,)), dma((2 * nz - 1,))],
        compiler_params=pltpu.CompilerParams(collective_id=0, has_side_effects=True),
        name="gather_keys",
    )(kv)


def attend_kernel(width, q_ref, kv_ref, o_ref):
    rows = q_ref.shape[0]
    factor = HEAD_SIZE ** (-0.5) * 1.4426950408889634
    q = q_ref[...]

    def step(i, state):
        top, total, acc = state
        at = pl.ds(pl.multiple_of(i * width, width), width)
        s = lax.dot_general(
            q, kv_ref[at, 0:HEAD_SIZE], (((1,), (1,)), ((), ())), preferred_element_type=F32
        )
        new_top = jnp.maximum(top, jnp.max(s, axis=1, keepdims=True))
        fade = jnp.exp2((top - new_top) * factor)
        w = jnp.exp2((s - new_top) * factor)
        total = total * fade + jnp.sum(w, axis=1, keepdims=True)
        acc = acc * fade + jnp.dot(
            w.astype(BF16), kv_ref[at, HEAD_SIZE:], preferred_element_type=F32
        )
        return new_top, total, acc

    start = (
        jnp.full((rows, 1), -1e30, F32), jnp.zeros((rows, 1), F32),
        jnp.zeros((rows, HEAD_SIZE), F32),
    )
    top, total, acc = lax.fori_loop(0, kv_ref.shape[0] // width, step, start, unroll=2)
    o_ref[...] = (acc / total).astype(BF16)


def attend(queries, kv):
    rows, columns = queries.shape
    heads = columns // HEAD_SIZE
    block = 256
    width = 1024
    keys = kv.shape[0]
    work = rows * heads * keys
    return pl.pallas_call(
        functools.partial(attend_kernel, width),
        out_shape=jax.ShapeDtypeStruct((rows, columns), BF16),
        grid=(heads, rows // block),
        in_specs=[
            pl.BlockSpec((block, HEAD_SIZE), lambda h, i: (i, h)),
            pl.BlockSpec((keys, kv.shape[1]), lambda h, i: (0, 0)),
        ],
        out_specs=pl.BlockSpec((block, HEAD_SIZE), lambda h, i: (i, h)),
        compiler_params=pltpu.CompilerParams(vmem_limit_bytes=VMEM_LIMIT),
        cost_estimate=pl.CostEstimate(
            flops=work * HEAD_SIZE * 4, bytes_accessed=keys * 512, transcendentals=work
        ),
        name="attend",
    )(queries, kv)


def norm_kernel(nx, proj_ref, res_ref, gain_ref, mid_ref, out_ref,
                from_core, outgo, from_x, squares, blocks, s1, r1, s2, r2, s3, r3, s4, r4, s5, r5):
    sp, tp, z, y, x, c = place()
    rows, own = res_ref.shape
    n_tp = 2 * nx
    other = x * 2 + 1 - c
    y_peer = z * 2 + 1 - y
    xs = [lax.rem(x + j, nx) for j in range(nx)]
    back = [lax.rem(x - j + nx, nx) for j in range(nx)]
    row_peers = [(sp, xs[j] * 2 + c) for j in range(1, nx)]
    cross = [(y_peer, xs[j] * 2 + c) for j in range(nx)]
    across = [(sp, xs[j] * 2 + 1 - c) for j in range(1, nx)]
    greet([(sp, other)] + row_peers + cross + across)

    def cols(t):
        return pl.ds(pl.multiple_of(t * own, own), own)

    step = rows // 8
    to_core = [
        remote(proj_ref.at[:, cols(xs[j] * 2 + 1 - c)], from_core.at[j],
               s1.at[j], r1.at[j], sp, other)
        for j in list(range(1, nx)) + [0]
    ]
    to_core = [to_core[-1]] + to_core[:-1]
    to_x = []
    for j in range(1, nx):
        to_core[j].wait_recv()

        @pl.loop(0, 8)
        def _(i):
            at = pl.ds(pl.multiple_of(i * step, step), step)
            outgo[j - 1, at, :] = (
                proj_ref[at, cols(xs[j] * 2 + c)].astype(F32) + from_core[j, at, :].astype(F32)
            ).astype(BF16)

        to_x.append(remote(outgo.at[j - 1], from_x.at[j - 1], s2.at[j - 1], r2.at[j - 1],
                           *row_peers[j - 1]))
    to_core[0].wait_recv()
    for copy in to_x:
        copy.wait_recv()
    ones = jnp.ones((8, own), F32)

    for i in range(rows // 256):
        at = pl.ds(i * 256, 256)
        total = proj_ref[at, cols(tp)].astype(F32) + from_core[0, at, :].astype(F32)
        for j in range(1, nx):
            total += from_x[j - 1, at, :].astype(F32)
        mid = res_ref[at, :].astype(F32) + total
        mid_ref[at, :] = mid
        squares[0, :, at] = lax.dot_general(
            ones, mid * mid, (((1,), (1,)), ((), ())),
            precision=lax.Precision.HIGHEST, preferred_element_type=F32,
        )
    peers = [(sp, other)] + row_peers + across
    sq = [
        remote(squares.at[0], squares.at[k + 1], s3.at[k], r3.at[k], *peers[k])
        for k in range(len(peers))
    ]
    for copy in sq:
        copy.wait_recv()
    for i in range(rows // 256):
        at = pl.ds(i * 256, 256)
        square = squares[0, :, at]
        for k in range(len(peers)):
            square += squares[k + 1, :, at]
        scale = lax.rsqrt(square.T[:, 0:1] / (n_tp * own) + eps)
        blocks[at, :] = (mid_ref[at, :] * scale * gain_ref[...]).astype(BF16)

    def spot(yy, t):
        return out_ref.at[pl.ds(pl.multiple_of(yy * rows, rows), rows), cols(t)]

    targets = cross + row_peers
    sources = [(1 - y, back[j] * 2 + c) for j in range(nx)]
    sources += [(y, back[j] * 2 + c) for j in range(1, nx)]
    mine = spot(y, tp)
    far = [
        remote(blocks, mine, s4.at[k], r4.at[k], *targets[k]) for k in range(len(targets))
    ]
    near = [remote(blocks, mine, s5.at[0], r5.at[0], sp, other)]
    out_ref[pl.ds(pl.multiple_of(y * rows, rows), rows), cols(tp)] = blocks[...]
    for k in range(len(targets)):
        far[k].wait_recv()
        block = spot(*sources[k])
        near.append(remote(block, block, s5.at[k + 1], r5.at[k + 1], sp, other))
    for copy in near:
        copy.wait_recv()
    for copy in to_core + to_x + sq + far + near:
        copy.wait_send()


def project_norm(proj, res, gain, n_tp):
    nx = n_tp // 2
    rows, own = res.shape
    dma = pltpu.SemaphoreType.DMA
    n = 2 * nx
    vm = pl.BlockSpec(memory_space=pltpu.VMEM)
    return pl.pallas_call(
        functools.partial(norm_kernel, nx),
        out_shape=(
            jax.ShapeDtypeStruct((rows, own), F32),
            jax.ShapeDtypeStruct((2 * rows, n_tp * own), BF16),
        ),
        in_specs=[vm] * 3,
        out_specs=(vm, vm),
        scratch_shapes=[
            pltpu.VMEM((nx, rows, own), BF16),
            pltpu.VMEM((nx - 1, rows, own), BF16),
            pltpu.VMEM((nx - 1, rows, own), BF16),
            pltpu.VMEM((n, 8, rows), F32),
            pltpu.VMEM((rows, own), BF16),
            dma((nx,)), dma((nx,)), dma((nx - 1,)), dma((nx - 1,)),
            dma((n - 1,)), dma((n - 1,)), dma((n - 1,)), dma((n - 1,)), dma((n,)), dma((n,)),
        ],
        compiler_params=pltpu.CompilerParams(
            collective_id=1, has_side_effects=True, vmem_limit_bytes=VMEM_LIMIT
        ),
        name="project_norm",
    )(proj, res, gain)


def down_kernel(nx, terms_ref, mid_ref, out_ref, from_core, outgo, arrived, s1, r1, s2, r2):
    sp, tp, z, y, x, c = place()
    rows, own = mid_ref.shape
    other = x * 2 + 1 - c
    y_peer = z * 2 + 1 - y
    xs = [lax.rem(x + j, nx) for j in range(nx)]
    targets = [(y_peer, 1 - y, xs[j]) for j in range(nx)] + [(sp, y, xs[j]) for j in range(1, nx)]
    peers = [(s, xx * 2 + c) for s, yy, xx in targets]
    greet([(sp, other)] + peers)

    def spot(yy, t):
        return (pl.ds(pl.multiple_of(yy * rows, rows), rows),
                pl.ds(pl.multiple_of(t * own, own), own))

    every = targets + [(sp, y, x)]
    near = [
        remote(terms_ref.at[spot(yy, xx * 2 + 1 - c)], from_core.at[k], s1.at[k], r1.at[k],
               sp, other)
        for k, (s, yy, xx) in enumerate(every)
    ]
    step = rows // 8
    far = []
    for k, (s, yy, xx) in enumerate(targets):
        near[k].wait_recv()

        @pl.loop(0, 8)
        def _(i):
            at = pl.ds(pl.multiple_of(i * step, step), step)
            here = pl.ds(pl.multiple_of(yy * rows + i * step, step), step)
            outgo[k, at, :] = (
                terms_ref[here, spot(yy, xx * 2 + c)[1]].astype(F32)
                + from_core[k, at, :].astype(F32)
            ).astype(BF16)

        far.append(remote(outgo.at[k], arrived.at[k], s2.at[k], r2.at[k], *peers[k]))
    near[-1].wait_recv()
    for copy in far:
        copy.wait_recv()

    @pl.loop(0, 8)
    def _(i):
        at = pl.ds(pl.multiple_of(i * step, step), step)
        here = pl.ds(pl.multiple_of(y * rows + i * step, step), step)
        total = terms_ref[here, spot(y, tp)[1]].astype(F32)
        total += from_core[len(targets), at, :].astype(F32)
        for k in range(len(targets)):
            total += arrived[k, at, :].astype(F32)
        out_ref[at, :] = (mid_ref[at, :] + 0.5 * total).astype(BF16)

    for copy in near + far:
        copy.wait_send()


def down_sum(terms, mid, n_tp):
    nx = n_tp // 2
    rows, own = mid.shape
    dma = pltpu.SemaphoreType.DMA
    n = 2 * nx
    vm = pl.BlockSpec(memory_space=pltpu.VMEM)
    return pl.pallas_call(
        functools.partial(down_kernel, nx),
        out_shape=jax.ShapeDtypeStruct((rows, own), BF16),
        in_specs=[vm] * 2,
        out_specs=vm,
        scratch_shapes=[
            pltpu.VMEM((n, rows, own), BF16),
            pltpu.VMEM((n - 1, rows, own), BF16),
            pltpu.VMEM((n - 1, rows, own), BF16),
            dma((n,)), dma((n,)), dma((n - 1,)), dma((n - 1,)),
        ],
        compiler_params=pltpu.CompilerParams(
            collective_id=2, has_side_effects=True, vmem_limit_bytes=VMEM_LIMIT
        ),
        name="down_sum",
    )(terms, mid)


def on_device(n_sp, n_tp, residual_in, queries, keys, values, query_gain, key_norm_gain,
              out_weight, mlp_gain, gate_weight, up_weight, down_weight):
    local_rows = residual_in.shape[0]
    local_heads = queries.shape[1] // HEAD_SIZE
    queries_per_group = QUERY_HEADS // KEY_VALUE_HEADS
    tp_index = lax.axis_index("tp")
    sp_index = lax.axis_index("sp")
    low = lax.rem(sp_index, 2)

    pairs = [(i, i ^ 1) for i in range(n_sp)]
    lanes = [[i for i in range(n_sp) if i % 2 == r] for r in range(2)]
    units = gate_weight.shape[1] // 2

    def halves(weight, axis):
        keep = lax.dynamic_slice_in_dim(weight, low * units, units, axis)
        give = lax.dynamic_slice_in_dim(weight, (1 - low) * units, units, axis)
        return keep, give

    gate_keep, gate_give = halves(gate_weight, 1)
    up_keep, up_give = halves(up_weight, 1)
    down_keep, down_give = halves(down_weight, 0)
    both_keep = jnp.concatenate([gate_keep, up_keep], axis=1)
    both_got = lax.ppermute(jnp.concatenate([gate_give, up_give], axis=1), "sp", pairs)
    down_got = lax.ppermute(down_give, "sp", pairs)

    def ordered(kept, got, axis):
        return jnp.where(
            low == 0,
            jnp.concatenate([kept, got], axis=axis),
            jnp.concatenate([got, kept], axis=axis),
        )

    both = lax.all_gather(
        ordered(both_keep, both_got, 0), "sp", axis=0, axis_index_groups=lanes, tiled=True
    )
    down = lax.all_gather(
        ordered(down_keep, down_got, 1), "sp", axis=1, axis_index_groups=lanes, tiled=True
    )

    grid_positions = sp_index * local_rows + jnp.arange(local_rows, dtype=jnp.int32)
    shared = tp_index * local_heads // queries_per_group
    own_keys = lax.dynamic_slice_in_dim(keys, shared * HEAD_SIZE, HEAD_SIZE, 1)
    own_values = lax.dynamic_slice_in_dim(values, shared * HEAD_SIZE, HEAD_SIZE, 1)
    key_matrix = apply_rotary(
        per_head_norm(own_keys.astype(F32)[:, None, :], key_norm_gain), grid_positions
    )[:, 0, :].astype(BF16)
    kv = gather_keys(jnp.concatenate([key_matrix, own_values], axis=1), n_sp)
    query_rows = apply_rotary(
        per_head_norm(queries.astype(F32).reshape(local_rows, local_heads, HEAD_SIZE), query_gain),
        grid_positions,
    ).astype(BF16).reshape(local_rows, local_heads * HEAD_SIZE)
    attended = attend(query_rows, kv)
    projected = jnp.dot(attended, out_weight, preferred_element_type=F32).astype(BF16)
    own_width = residual_in.shape[1]
    gain_own = lax.dynamic_slice_in_dim(mlp_gain, tp_index * own_width, own_width, 0)[None, :]
    residual_mid, normed = project_norm(projected, residual_in, gain_own, n_tp)
    gate_up = jnp.dot(normed, both, preferred_element_type=F32)
    hidden = (jax.nn.silu(gate_up[:, :units]) * gate_up[:, units:]).astype(BF16)
    down_terms = jnp.dot(hidden, down, preferred_element_type=F32).astype(BF16)
    return down_sum(down_terms, residual_mid, n_tp)


def solution(mesh):
    in_specs = (
        P("sp", "tp"),
        P("sp", "tp"),
        P("sp", None),
        P("sp", None),
        P(),
        P(),
        P("tp", None),
        P(),
        P("sp", "tp"),
        P("sp", "tp"),
        P("tp", "sp"),
    )
    out_specs = P("sp", "tp")
    return jax.shard_map(
        functools.partial(on_device, mesh.shape["sp"], mesh.shape["tp"]),
        mesh=mesh, in_specs=in_specs, out_specs=out_specs, check_vma=False,
    )
```

```python
import functools
import jax
import jax.numpy as jnp
from jax import lax
from jax.experimental import pallas as pl
from jax.experimental.pallas import tpu as pltpu
from jax.sharding import PartitionSpec as P

D = 2048
HEAD_SIZE = 128
QUERY_HEADS = 8
KEY_VALUE_HEADS = 2
GRID = 64

eps = 1e-06
rotary_base = 10000.0
MESH = pl.DeviceIdType.MESH
VMEM_LIMIT = 60 * 1024 * 1024
F32 = jnp.float32
BF16 = jnp.bfloat16


def apply_rotary(vectors, grid_positions):
    half_size = vectors.shape[-1] // 2
    frequency = rotary_base ** (-jnp.arange(0, half_size, 2, dtype=F32) / half_size)
    grid_row = (grid_positions // GRID).astype(F32)
    grid_col = (grid_positions % GRID).astype(F32)
    angles = jnp.concatenate(
        [grid_row[:, None] * frequency, grid_col[:, None] * frequency], axis=-1
    )[:, None, :]
    cosine_table = jnp.cos(angles)
    sine_table = jnp.sin(angles)
    first_half = vectors[..., :half_size]
    second_half = vectors[..., half_size:]
    return jnp.concatenate(
        [
            first_half * cosine_table - second_half * sine_table,
            first_half * sine_table + second_half * cosine_table,
        ],
        axis=-1,
    )


def per_head_norm(vectors, gain):
    return vectors * lax.rsqrt(jnp.mean(vectors * vectors, axis=-1, keepdims=True) + eps) * gain


def remote(src, dst, send, recv, sp, tp):
    copy = pltpu.make_async_remote_copy(
        src_ref=src, dst_ref=dst, send_sem=send, recv_sem=recv,
        device_id={"sp": sp, "tp": tp}, device_id_type=MESH,
    )
    copy.start()
    return copy


def greet(peers):
    barrier = pltpu.get_barrier_semaphore()
    for sp, tp in peers:
        pl.semaphore_signal(
            barrier, inc=1, device_id={"sp": sp, "tp": tp}, device_id_type=MESH
        )
    pl.semaphore_wait(barrier, len(peers))


def place():
    sp = lax.axis_index("sp")
    tp = lax.axis_index("tp")
    return sp, tp, sp // 2, lax.rem(sp, 2), tp // 2, lax.rem(tp, 2)


def gather_kernel(nz, kv_ref, out_ref, sz, rz, sy, ry, sc, rc):
    sp, tp, z, y, x, c = place()
    rows = kv_ref.shape[0]
    half = rows // 2
    other = x * 2 + (1 - c)
    z_peers = [lax.rem(z + k, nz) * 2 + y for k in range(1, nz)]
    y_peer = z * 2 + 1 - y
    greet([(p, tp) for p in z_peers] + [(y_peer, tp), (sp, other)])

    def spot(owner):
        return out_ref.at[pl.ds(pl.multiple_of(owner * rows + c * half, half), half), :]

    own = kv_ref.at[pl.ds(pl.multiple_of(c * half, half), half), :]
    sends = []
    to_z = [
        remote(own, spot(sp), sz.at[k - 1], rz.at[k - 1], z_peers[k - 1], tp)
        for k in range(1, nz)
    ]
    to_y = [remote(own, spot(sp), sy.at[0], ry.at[0], y_peer, tp)]
    out_ref[pl.ds(pl.multiple_of(sp * rows, rows), rows), :] = kv_ref[...]
    to_core = []
    for k in range(1, nz):
        to_z[k - 1].wait_recv()
        block = spot(lax.rem(z - k + nz, nz) * 2 + y)
        to_y.append(remote(block, block, sy.at[k], ry.at[k], y_peer, tp))
        to_core.append(remote(block, block, sc.at[k - 1], rc.at[k - 1], sp, other))
    for k in range(nz):
        to_y[k].wait_recv()
        block = spot(lax.rem(z - k + nz, nz) * 2 + 1 - y)
        slot = nz - 1 + k
        to_core.append(remote(block, block, sc.at[slot], rc.at[slot], sp, other))
    for copy in to_core:
        copy.wait_recv()
    for copy in to_z + to_y + to_core:
        copy.wait_send()


def gather_keys(kv, n_sp):
    nz = n_sp // 2
    dma = pltpu.SemaphoreType.DMA
    return pl.pallas_call(
        functools.partial(gather_kernel, nz),
        out_shape=jax.ShapeDtypeStruct((n_sp * kv.shape[0], kv.shape[1]), kv.dtype),
        in_specs=[pl.BlockSpec(memory_space=pltpu.VMEM)],
        out_specs=pl.BlockSpec(memory_space=pltpu.VMEM),
        scratch_shapes=[dma((nz - 1,)), dma((nz - 1,)), dma((nz,)), dma((nz,)),
                        dma((2 * nz - 1,)), dma((2 * nz - 1,))],
        compiler_params=pltpu.CompilerParams(collective_id=0, has_side_effects=True),
        name="gather_keys",
    )(kv)


def attend_kernel(width, q_ref, kv_ref, o_ref):
    rows = q_ref.shape[0]
    factor = HEAD_SIZE ** (-0.5) * 1.4426950408889634
    q = q_ref[...]

    def step(i, state):
        top, total, acc = state
        at = pl.ds(pl.multiple_of(i * width, width), width)
        s = lax.dot_general(
            q, kv_ref[at, 0:HEAD_SIZE], (((1,), (1,)), ((), ())), preferred_element_type=F32
        )
        new_top = jnp.maximum(top, jnp.max(s, axis=1, keepdims=True))
        fade = jnp.exp2((top - new_top) * factor)
        w = jnp.exp2((s - new_top) * factor)
        total = total * fade + jnp.sum(w, axis=1, keepdims=True)
        acc = acc * fade + jnp.dot(
            w.astype(BF16), kv_ref[at, HEAD_SIZE:], preferred_element_type=F32
        )
        return new_top, total, acc

    start = (
        jnp.full((rows, 1), -1e30, F32), jnp.zeros((rows, 1), F32),
        jnp.zeros((rows, HEAD_SIZE), F32),
    )
    top, total, acc = lax.fori_loop(0, kv_ref.shape[0] // width, step, start, unroll=2)
    o_ref[...] = (acc / total).astype(BF16)


def attend(queries, kv):
    rows, columns = queries.shape
    heads = columns // HEAD_SIZE
    block = 256
    width = 1024
    keys = kv.shape[0]
    work = rows * heads * keys
    return pl.pallas_call(
        functools.partial(attend_kernel, width),
        out_shape=jax.ShapeDtypeStruct((rows, columns), BF16),
        grid=(heads, rows // block),
        in_specs=[
            pl.BlockSpec((block, HEAD_SIZE), lambda h, i: (i, h)),
            pl.BlockSpec((keys, kv.shape[1]), lambda h, i: (0, 0)),
        ],
        out_specs=pl.BlockSpec((block, HEAD_SIZE), lambda h, i: (i, h)),
        compiler_params=pltpu.CompilerParams(vmem_limit_bytes=VMEM_LIMIT),
        cost_estimate=pl.CostEstimate(
            flops=work * HEAD_SIZE * 4, bytes_accessed=keys * 512, transcendentals=work
        ),
        name="attend",
    )(queries, kv)


def norm_kernel(nx, proj_ref, res_ref, gain_ref, mid_ref, out_ref,
                from_core, outgo, from_x, squares, blocks, s1, r1, s2, r2, s3, r3, s4, r4, s5, r5):
    sp, tp, z, y, x, c = place()
    rows, own = res_ref.shape
    n_tp = 2 * nx
    other = x * 2 + 1 - c
    y_peer = z * 2 + 1 - y
    xs = [lax.rem(x + j, nx) for j in range(nx)]
    back = [lax.rem(x - j + nx, nx) for j in range(nx)]
    row_peers = [(sp, xs[j] * 2 + c) for j in range(1, nx)]
    cross = [(y_peer, xs[j] * 2 + c) for j in range(nx)]
    across = [(sp, xs[j] * 2 + 1 - c) for j in range(1, nx)]
    greet([(sp, other)] + row_peers + cross + across)

    def cols(t):
        return pl.ds(pl.multiple_of(t * own, own), own)

    step = rows // 8
    to_core = [
        remote(proj_ref.at[:, cols(xs[j] * 2 + 1 - c)], from_core.at[j],
               s1.at[j], r1.at[j], sp, other)
        for j in list(range(1, nx)) + [0]
    ]
    to_core = [to_core[-1]] + to_core[:-1]
    to_x = []
    for j in range(1, nx):
        to_core[j].wait_recv()

        @pl.loop(0, 8)
        def _(i):
            at = pl.ds(pl.multiple_of(i * step, step), step)
            outgo[j - 1, at, :] = (
                proj_ref[at, cols(xs[j] * 2 + c)].astype(F32) + from_core[j, at, :].astype(F32)
            ).astype(BF16)

        to_x.append(remote(outgo.at[j - 1], from_x.at[j - 1], s2.at[j - 1], r2.at[j - 1],
                           *row_peers[j - 1]))
    to_core[0].wait_recv()
    for copy in to_x:
        copy.wait_recv()
    ones = jnp.ones((8, own), F32)

    for i in range(rows // 256):
        at = pl.ds(i * 256, 256)
        total = proj_ref[at, cols(tp)].astype(F32) + from_core[0, at, :].astype(F32)
        for j in range(1, nx):
            total += from_x[j - 1, at, :].astype(F32)
        mid = res_ref[at, :].astype(F32) + total
        mid_ref[at, :] = mid
        squares[0, :, at] = lax.dot_general(
            ones, mid * mid, (((1,), (1,)), ((), ())),
            precision=lax.Precision.HIGHEST, preferred_element_type=F32,
        )
    peers = [(sp, other)] + row_peers + across
    sq = [
        remote(squares.at[0], squares.at[k + 1], s3.at[k], r3.at[k], *peers[k])
        for k in range(len(peers))
    ]
    for copy in sq:
        copy.wait_recv()
    for i in range(rows // 256):
        at = pl.ds(i * 256, 256)
        square = squares[0, :, at]
        for k in range(len(peers)):
            square += squares[k + 1, :, at]
        scale = lax.rsqrt(square.T[:, 0:1] / (n_tp * own) + eps)
        block = (mid_ref[at, :] * scale * gain_ref[...]).astype(BF16)
        blocks[0, at, :] = block[:, : own // 2]
        blocks[1, at, :] = block[:, own // 2 :]

    half = own // 2

    def spot(yy, t):
        return (pl.ds(pl.multiple_of(yy * rows, rows), rows),
                pl.ds(pl.multiple_of(t * half, half), half))

    targets = cross + row_peers
    sources = [(1 - y, back[j] * 2 + c) for j in range(nx)]
    sources += [(y, back[j] * 2 + c) for j in range(1, nx)]
    mine = spot(y, tp)
    far = []
    for k in range(len(targets)):
        side = 1 - y if k < nx else y
        for i in range(2):
            at = (lax.rem(i + side, 2),) + mine
            far.append(remote(blocks.at[i], out_ref.at[at], s4.at[2 * k + i], r4.at[2 * k + i],
                              *targets[k]))
    near = []
    for i in range(2):
        at = (lax.rem(i + y, 2),) + mine
        near.append(remote(blocks.at[i], out_ref.at[at], s5.at[i], r5.at[i], sp, other))
        out_ref[at] = blocks[i]
    for k in range(len(targets)):
        for i in range(2):
            far[2 * k + i].wait_recv()
            at = (lax.rem(i + y, 2),) + spot(*sources[k])
            slot = 2 * k + 2 + i
            near.append(remote(out_ref.at[at], out_ref.at[at], s5.at[slot], r5.at[slot], sp, other))
    for copy in near:
        copy.wait_recv()
    for copy in to_core + to_x + sq + far + near:
        copy.wait_send()


def project_norm(proj, res, gain, n_tp):
    nx = n_tp // 2
    rows, own = res.shape
    dma = pltpu.SemaphoreType.DMA
    n = 2 * nx
    vm = pl.BlockSpec(memory_space=pltpu.VMEM)
    return pl.pallas_call(
        functools.partial(norm_kernel, nx),
        out_shape=(
            jax.ShapeDtypeStruct((rows, own), F32),
            jax.ShapeDtypeStruct((2, 2 * rows, n_tp * own // 2), BF16),
        ),
        in_specs=[vm] * 3,
        out_specs=(vm, vm),
        scratch_shapes=[
            pltpu.VMEM((nx, rows, own), BF16),
            pltpu.VMEM((nx - 1, rows, own), BF16),
            pltpu.VMEM((nx - 1, rows, own), BF16),
            pltpu.VMEM((n, 8, rows), F32),
            pltpu.VMEM((2, rows, own // 2), BF16),
            dma((nx,)), dma((nx,)), dma((nx - 1,)), dma((nx - 1,)),
            dma((n - 1,)), dma((n - 1,)), dma((2 * n - 2,)), dma((2 * n - 2,)),
            dma((2 * n,)), dma((2 * n,)),
        ],
        compiler_params=pltpu.CompilerParams(
            collective_id=1, has_side_effects=True, vmem_limit_bytes=VMEM_LIMIT
        ),
        name="project_norm",
    )(proj, res, gain)


def down_kernel(nx, terms_ref, mid_ref, out_ref, from_core, outgo, from_y, from_x, relay,
                last_x, last_y, s1, r1, s2, r2, s3, r3, s4, r4, s5, r5):
    sp, tp, z, y, x, c = place()
    rows, own = mid_ref.shape
    half = rows // 2
    top, low = pl.ds(0, half), pl.ds(half, half)
    other = x * 2 + 1 - c
    y_peer = (z * 2 + 1 - y, tp)
    xs = [lax.rem(x + j, nx) for j in range(nx)]
    x_peers = [(sp, xs[j] * 2 + c) for j in range(nx)]
    greet([(sp, other), y_peer] + x_peers[1:])
    every = [(1 - y, xs[j]) for j in range(nx)] + [(y, xs[j]) for j in range(1, nx)] + [(y, x)]
    order = list(range(1, 2 * nx - 1)) + [0, 2 * nx - 1]

    def cols(t):
        return pl.ds(pl.multiple_of(t * own, own), own)

    near = {}
    for k in order:
        yy, xx = every[k]
        near[k] = remote(
            terms_ref.at[pl.ds(pl.multiple_of(yy * rows, rows), rows), cols(xx * 2 + 1 - c)],
            from_core.at[k], s1.at[k], r1.at[k], sp, other)
    step = rows // 8
    to_y, to_x, again = {}, {}, []
    for k in order[:-1]:
        yy, xx = every[k]
        near[k].wait_recv()

        @pl.loop(0, 8)
        def _(i):
            at = pl.ds(pl.multiple_of(i * step, step), step)
            here = pl.ds(pl.multiple_of(yy * rows + i * step, step), step)
            outgo[k, at, :] = (
                terms_ref[here, cols(xx * 2 + c)].astype(F32) + from_core[k, at, :].astype(F32)
            ).astype(BF16)

        if k < nx:
            to_y[k] = remote(outgo.at[k, top], from_y.at[k], s2.at[k], r2.at[k], *y_peer)
        j = k if k < nx else k - nx + 1
        if j > 0:
            slot = 2 * (j - 1) + (1 if k < nx else 0)
            to_x[slot] = remote(outgo.at[k, low], from_x.at[slot], s3.at[slot], r3.at[slot],
                                *x_peers[j])
    for j in range(1, nx):
        to_y[j].wait_recv()

        @pl.loop(0, 4)
        def _(i):
            at = pl.ds(pl.multiple_of(i * step, step), step)
            relay[j, at, :] = (
                outgo[nx + j - 1, at, :].astype(F32) + from_y[j, at, :].astype(F32)
            ).astype(BF16)

        again.append(remote(relay.at[j], last_x.at[j - 1], s4.at[j - 1], r4.at[j - 1],
                            *x_peers[j]))
    for j in range(1, nx):
        to_x[2 * j - 1].wait_recv()

    @pl.loop(0, 4)
    def _(i):
        at = pl.ds(pl.multiple_of(i * step, step), step)
        here = pl.ds(pl.multiple_of(half + i * step, step), step)
        total = outgo[0, here, :].astype(F32)
        for j in range(1, nx):
            total += from_x[2 * j - 1, at, :].astype(F32)
        relay[0, at, :] = total.astype(BF16)

    again.append(remote(relay.at[0], last_y, s5.at[0], r5.at[0], *y_peer))
    near[2 * nx - 1].wait_recv()
    to_y[0].wait_recv()
    for j in range(1, nx):
        to_x[2 * j - 2].wait_recv()
    for copy in again:
        copy.wait_recv()

    @pl.loop(0, 4)
    def _(i):
        at = pl.ds(pl.multiple_of(i * step, step), step)
        for part in range(2):
            to = pl.ds(pl.multiple_of(part * half + i * step, step), step)
            here = pl.ds(pl.multiple_of(y * rows + part * half + i * step, step), step)
            total = terms_ref[here, cols(tp)].astype(F32)
            total += from_core[2 * nx - 1, to, :].astype(F32)
            total += (from_y[0, at, :] if part == 0 else last_y[at, :]).astype(F32)
            for j in range(1, nx):
                total += (last_x[j - 1, at, :] if part == 0
                          else from_x[2 * j - 2, at, :]).astype(F32)
            out_ref[to, :] = (mid_ref[to, :] + 0.5 * total).astype(BF16)

    for copy in list(near.values()) + list(to_y.values()) + list(to_x.values()) + again:
        copy.wait_send()


def down_sum(terms, mid, n_tp):
    nx = n_tp // 2
    rows, own = mid.shape
    dma = pltpu.SemaphoreType.DMA
    n = 2 * nx
    vm = pl.BlockSpec(memory_space=pltpu.VMEM)
    return pl.pallas_call(
        functools.partial(down_kernel, nx),
        out_shape=jax.ShapeDtypeStruct((rows, own), BF16),
        in_specs=[vm] * 2,
        out_specs=vm,
        scratch_shapes=[
            pltpu.VMEM((n, rows, own), BF16),
            pltpu.VMEM((n - 1, rows, own), BF16),
            pltpu.VMEM((nx, rows // 2, own), BF16),
            pltpu.VMEM((n - 2, rows // 2, own), BF16),
            pltpu.VMEM((nx, rows // 2, own), BF16),
            pltpu.VMEM((nx - 1, rows // 2, own), BF16),
            pltpu.VMEM((rows // 2, own), BF16),
            dma((n,)), dma((n,)), dma((nx,)), dma((nx,)), dma((n - 2,)), dma((n - 2,)),
            dma((nx - 1,)), dma((nx - 1,)), dma((1,)), dma((1,)),
        ],
        compiler_params=pltpu.CompilerParams(
            collective_id=2, has_side_effects=True, vmem_limit_bytes=VMEM_LIMIT
        ),
        name="down_sum",
    )(terms, mid)


def on_device(n_sp, n_tp, residual_in, queries, keys, values, query_gain, key_norm_gain,
              out_weight, mlp_gain, gate_weight, up_weight, down_weight):
    local_rows = residual_in.shape[0]
    local_heads = queries.shape[1] // HEAD_SIZE
    queries_per_group = QUERY_HEADS // KEY_VALUE_HEADS
    tp_index = lax.axis_index("tp")
    sp_index = lax.axis_index("sp")
    low = lax.rem(sp_index, 2)

    pairs = [(i, i ^ 1) for i in range(n_sp)]
    lanes = [[i for i in range(n_sp) if i % 2 == r] for r in range(2)]
    units = gate_weight.shape[1] // 2

    def halves(weight, axis):
        keep = lax.dynamic_slice_in_dim(weight, low * units, units, axis)
        give = lax.dynamic_slice_in_dim(weight, (1 - low) * units, units, axis)
        return keep, give

    gate_keep, gate_give = halves(gate_weight, 1)
    up_keep, up_give = halves(up_weight, 1)
    down_keep, down_give = halves(down_weight, 0)
    both_keep = jnp.concatenate([gate_keep, up_keep], axis=1)
    both_got = lax.ppermute(jnp.concatenate([gate_give, up_give], axis=1), "sp", pairs)
    down_got = lax.ppermute(down_give, "sp", pairs)

    def ordered(kept, got, axis):
        return jnp.where(
            low == 0,
            jnp.concatenate([kept, got], axis=axis),
            jnp.concatenate([got, kept], axis=axis),
        )

    both_first = lax.all_gather(
        both_keep, "sp", axis=0, axis_index_groups=lanes, tiled=True
    )
    grid_positions = sp_index * local_rows + jnp.arange(local_rows, dtype=jnp.int32)
    shared = tp_index * local_heads // queries_per_group
    own_keys = lax.dynamic_slice_in_dim(keys, shared * HEAD_SIZE, HEAD_SIZE, 1)
    own_values = lax.dynamic_slice_in_dim(values, shared * HEAD_SIZE, HEAD_SIZE, 1)
    key_matrix = apply_rotary(
        per_head_norm(own_keys.astype(F32)[:, None, :], key_norm_gain), grid_positions
    )[:, 0, :].astype(BF16)
    query_rows = apply_rotary(
        per_head_norm(queries.astype(F32).reshape(local_rows, local_heads, HEAD_SIZE), query_gain),
        grid_positions,
    ).astype(BF16).reshape(local_rows, local_heads * HEAD_SIZE)
    own_kv, query_rows, both_got, down_got = lax.optimization_barrier(
        (jnp.concatenate([key_matrix, own_values], axis=1), query_rows, both_got, down_got)
    )
    both_second = lax.all_gather(
        both_got, "sp", axis=0, axis_index_groups=lanes, tiled=True
    )
    down = lax.all_gather(
        ordered(down_keep, down_got, 1), "sp", axis=1, axis_index_groups=lanes, tiled=True
    )
    kv = gather_keys(own_kv, n_sp)
    attended = attend(query_rows, kv)
    projected = jnp.dot(attended, out_weight, preferred_element_type=F32).astype(BF16)
    own_width = residual_in.shape[1]
    gain_own = lax.dynamic_slice_in_dim(mlp_gain, tp_index * own_width, own_width, 0)[None, :]
    residual_mid, normed = project_norm(projected, residual_in, gain_own, n_tp)
    assert n_sp == 2 * n_tp
    gate_up = jnp.dot(normed[0], both_first, preferred_element_type=F32)
    gate_up += jnp.dot(normed[1], both_second, preferred_element_type=F32)
    hidden = (jax.nn.silu(gate_up[:, :units]) * gate_up[:, units:]).astype(BF16)
    down_terms = jnp.dot(hidden, down, preferred_element_type=F32).astype(BF16)
    return down_sum(down_terms, residual_mid, n_tp)


def solution(mesh):
    in_specs = (
        P("sp", "tp"),
        P("sp", "tp"),
        P("sp", None),
        P("sp", None),
        P(),
        P(),
        P("tp", None),
        P(),
        P("sp", "tp"),
        P("sp", "tp"),
        P("tp", "sp"),
    )
    out_specs = P("sp", "tp")
    return jax.shard_map(
        functools.partial(on_device, mesh.shape["sp"], mesh.shape["tp"]),
        mesh=mesh, in_specs=in_specs, out_specs=out_specs, check_vma=False,
    )
```
